32 devices in a mesh: fs: 8 (over z, y), tp: 4 (over x, core).
Axes of the slice: x: 2, y: 2, z: 4, core: 2. Of those that a mesh axis runs over, the one named last changes fastest.
Arguments:
- resid: bfloat16 [12288, 2048], P(('fs', 'tp')), may hold values from -6 to 6
- norm1_gain: float32 [2048], replicated, may hold values from 0.1 to 1.9
- w_value: float32 [2048, 2048], P('fs', 'tp'), may hold values from -0.125 to 0.125
- w_gate: float32 [2048, 2048], P('fs', 'tp'), may hold values from -0.125 to 0.125
- value_scale: float32 [2048], replicated, may hold values from 0.3 to 3
- gate_scale: float32 [2048], replicated, may hold values from 0.5 to 3
- conv_taps: float32 [31, 2048], replicated, may hold values from -1 to 1
- conv_gain: float32 [2048], replicated, may hold values from 0.1 to 1.9
- w_point: float32 [2048, 2048], P('tp', 'fs'), may hold values from -0.125 to 0.125
- point_scale: float32 [2048], P('fs'), may hold values from 0.5 to 3
- norm2_gain: float32 [2048], replicated, may hold values from 0.1 to 1.9
- w_up: float32 [2048, 8192], P('fs', 'tp'), may hold values from -0.125 to 0.125
- up_scale: float32 [8192], P('tp'), may hold values from 0.5 to 1.5
- w_down: float32 [8192, 2048], P('tp', 'fs'), may hold values from -0.0625 to 0.0625
- down_scale: float32 [2048], P('fs'), may hold values from 0.3 to 1
Outputs:
- layer_out: bfloat16 [12288, 2048], P(('fs', 'tp'))
The draws below stay inside these ranges and needn't reach their ends.
All inputs are finite; a program needn't handle non-finite values.
Results may differ from the reference program's by a relative error of at most 0.015.
Values may be sent and summed in bfloat16 or wider, within the bound.
No kernel may reach another device: no remote copies, remote signals or barrier semaphores. Data moves between devices by JAX's collectives and lax.ppermute only.
A program may use at most 128 MiB of HBM per device.

```python
import math
import jax
import jax.numpy as jnp
from jax import lax

D = 2048
CH = 2048
FF = 8192
KERNEL = 31
GROUPS = 4
LEN = 1536
TOKENS = 12288
N_TP = 4


def levels(stream_key, extent, shards, low, top_value):
    level = 1.0
    for position, shards_of in shards:
        heights = jax.random.uniform(jax.random.fold_in(jax.random.fold_in(stream_key, 6), position), (shards_of,), jnp.float32, low / len(shards), top_value / len(shards))
        level = level * jnp.repeat(jnp.exp(heights), extent[position] // shards_of).reshape((-1,) + (1,) * (len(extent) - 1 - position))
    return level


def noise(own_key, extent, scale, most, pieces=(), kind=jnp.bfloat16):
    entries = scale * jax.random.normal(own_key, extent, jnp.float32)
    if pieces:
        entries = entries * levels(own_key, extent, pieces, -0.22, 0.18)
    return jnp.clip(entries, -most, most).astype(kind)


def setup_inputs(seed: int = 0) -> dict:
    key_list = jax.random.split(jax.random.key(seed), 16)
    return {
        "resid": noise(key_list[0], (TOKENS, D), 1.0, 6.0, ((0, 32),)),
        "norm1_gain": jnp.clip(1.0 + 0.18 * jax.random.normal(key_list[1], (D,), jnp.float32), 0.1, 1.9),
        "w_value": noise(key_list[2], (D, CH), D ** -0.5, 0.125, ((0, 8), (1, 4)), jnp.float32),
        "w_gate": noise(key_list[3], (D, CH), D ** -0.5, 0.125, ((0, 8), (1, 4)), jnp.float32),
        "value_scale": jnp.clip(jnp.exp(jax.random.uniform(key_list[4], (CH,), jnp.float32, math.log(0.3), math.log(3.0))), 0.3, 3.0),
        "gate_scale": jnp.clip(jnp.exp(jax.random.uniform(key_list[5], (CH,), jnp.float32, math.log(0.5), math.log(3.0))), 0.5, 3.0),
        "conv_taps": noise(key_list[6], (KERNEL, CH), KERNEL ** -0.5, 1.0, (), jnp.float32),
        "conv_gain": jnp.clip(1.0 + 0.18 * jax.random.normal(key_list[7], (CH,), jnp.float32), 0.1, 1.9),
        "w_point": noise(key_list[8], (CH, D), CH ** -0.5, 0.125, ((0, 4), (1, 8)), jnp.float32),
        "point_scale": jnp.clip(jnp.exp(math.log(3.0) - 1.7917595 * jax.random.uniform(key_list[9], (D,), jnp.float32) ** levels(key_list[9], (D,), ((0, 8),), -0.2, 0.2)), 0.5, 3.0),
        "norm2_gain": jnp.clip(1.0 + 0.18 * jax.random.normal(key_list[10], (D,), jnp.float32), 0.1, 1.9),
        "w_up": noise(key_list[11], (D, FF), D ** -0.5, 0.125, ((0, 8), (1, 4)), jnp.float32),
        "up_scale": jnp.clip(jnp.exp(math.log(1.5) - 1.0986123 * jax.random.uniform(key_list[12], (FF,), jnp.float32) ** levels(key_list[12], (FF,), ((0, 4),), -0.2, 0.2)), 0.5, 1.5),
        "w_down": noise(key_list[13], (FF, D), FF ** -0.5, 0.0625, ((0, 4), (1, 8)), jnp.float32),
        "down_scale": jnp.clip(jnp.exp(math.log(1.0) - 1.2039728 * jax.random.uniform(key_list[14], (D,), jnp.float32) ** levels(key_list[14], (D,), ((0, 8),), -0.2, 0.2)), 0.3, 1.0),
    }


def rms_scaled(values, gain):
    data = values.astype(jnp.float32)
    return data * lax.rsqrt(lax.optimization_barrier(jnp.mean(data * data, axis=-1, keepdims=True)) + 1e-06) * gain

def reference(resid, norm1_gain, w_value, w_gate, value_scale, gate_scale, conv_taps, conv_gain, w_point, point_scale, norm2_gain, w_up, up_scale, w_down, down_scale):
    value_bf = w_value.astype(jnp.bfloat16)
    gate_bf = w_gate.astype(jnp.bfloat16)
    point_bf = w_point.astype(jnp.bfloat16)
    up_bf = w_up.astype(jnp.bfloat16)
    down_bf = w_down.astype(jnp.bfloat16)
    normed = rms_scaled(resid, norm1_gain).astype(jnp.bfloat16)
    value = jnp.dot(normed, value_bf, preferred_element_type=jnp.float32) * value_scale
    gate = jnp.dot(normed, gate_bf, preferred_element_type=jnp.float32) * gate_scale
    glu = (value * jax.nn.sigmoid(gate)).astype(jnp.bfloat16)
    reach = KERNEL // 2
    seqs = glu.reshape(-1, LEN, CH).astype(jnp.float32)
    padded = jnp.pad(seqs, ((0, 0), (reach, reach), (0, 0)))
    conv = jnp.zeros(seqs.shape, jnp.float32)
    for offset in range(KERNEL):
        conv = conv + conv_taps[offset] * padded[:, offset:offset + LEN]
    grouped = conv.reshape(-1, CH // GROUPS, GROUPS)
    gmean = lax.optimization_barrier(jnp.mean(grouped, axis=-2, keepdims=True))
    gsquare = lax.optimization_barrier(jnp.mean(grouped * grouped, axis=-2, keepdims=True))
    scaled = ((grouped - gmean) * lax.rsqrt(gsquare - gmean * gmean + 1e-05)).reshape(-1, CH) * conv_gain
    act = jax.nn.silu(scaled).astype(jnp.bfloat16)
    mixed = jnp.dot(act, point_bf, preferred_element_type=jnp.float32) * point_scale
    middle = (resid.astype(jnp.float32) + mixed).astype(jnp.bfloat16)
    normed2 = rms_scaled(middle, norm2_gain).astype(jnp.bfloat16)
    upper = jnp.dot(normed2, up_bf, preferred_element_type=jnp.float32) * up_scale
    hidden = jnp.square(jax.nn.relu(upper)).astype(jnp.bfloat16)
    block = FF // N_TP
    hid_blocks = jnp.transpose(hidden.reshape(hidden.shape[0], N_TP, block), (1, 0, 2))
    down_blocks = down_bf.reshape(N_TP, block, D)

    def add_block(total, pair):
        hid_block, down_block = pair
        partial_value = (jnp.dot(hid_block, down_block, preferred_element_type=jnp.float32) * down_scale).astype(jnp.bfloat16)
        partial_value = lax.optimization_barrier(partial_value)
        return (total + partial_value.astype(jnp.float32), None)
    total, _ = lax.scan(add_block, jnp.zeros((hidden.shape[0], D), jnp.float32), (hid_blocks, down_blocks))
    return (middle.astype(jnp.float32) + total).astype(jnp.bfloat16)
```

```python
import functools
import math

import jax
import jax.numpy as jnp
import numpy as np
from jax import lax
from jax.experimental import pallas as pl
from jax.experimental.pallas import tpu as pltpu
from jax.sharding import PartitionSpec as P

GROUPS = 4
LANES = 128
F32 = jnp.float32
BF16 = jnp.bfloat16


def ring_order(fs_count, tp_count):
    cols = tp_count // 2
    if cols < 2 or fs_count % cols or (fs_count // cols) % 2:
        return list(range(fs_count))
    rows = fs_count // cols
    order = []
    for z in range(rows):
        ys = range(1, cols) if z % 2 == 0 else range(cols - 1, 0, -1)
        order += [z * cols + y for y in ys]
    return order + [z * cols for z in reversed(range(rows))]


class Plan:
    def __init__(self, fs_count, tp_count):
        self.fs, self.tp = fs_count, tp_count
        self.chips = tp_count // 2
        self.order = ring_order(fs_count, tp_count)
        self.hops = fs_count // 2
        n = fs_count
        self.fwd = [(self.order[i], self.order[(i + 1) % n]) for i in range(n)]
        self.bwd = [(self.order[(i + 1) % n], self.order[i]) for i in range(n)]
        self.offsets = [0]
        for k in range(1, self.hops):
            self.offsets += [-k, k]
        self.offsets.append(self.hops)
        self.core_swap = [(i, i ^ 1) for i in range(tp_count)]

    def shift(self, d):
        return [(i, (i + 2 * d) % self.tp) for i in range(self.tp)]

    def table(self):
        place = {dev: i for i, dev in enumerate(self.order)}
        rows = []
        for f in range(self.fs):
            owners = [self.order[(place[f] + o) % self.fs] for o in self.offsets]
            for t in range(self.tp):
                chip, core = divmod(t, 2)
                pieces = []
                for s in range(self.chips):
                    base = ((chip + s) % self.chips) * 2
                    pieces += [base + core, base + 1 - core]
                rows.append(owners + pieces + [t])
        return np.asarray(rows, np.int32)


def call(kernel, meta, ins, outs, scratch, flops, name):
    specs = [pl.BlockSpec(memory_space=pltpu.HBM if hbm else pltpu.VMEM) for _, hbm in ins]
    moved = sum(a.size * a.dtype.itemsize for a, _ in ins) + sum(math.prod(s) * jnp.dtype(d).itemsize for s, d in outs)
    with jax.named_scope(name):
        return pl.pallas_call(
            kernel,
            name=name,
            out_shape=[jax.ShapeDtypeStruct(s, d) for s, d in outs],
            in_specs=[pl.BlockSpec(memory_space=pltpu.SMEM)] + specs,
            out_specs=[pl.BlockSpec(memory_space=pltpu.VMEM) for _ in outs],
            scratch_shapes=scratch,
            compiler_params=pltpu.CompilerParams(vmem_limit_bytes=60 * 1024 * 1024),
            cost_estimate=pl.CostEstimate(flops=int(flops), bytes_accessed=int(moved), transcendentals=0),
        )(meta, *[a for a, _ in ins])


class Parts:
    def __init__(self, parts, shape):
        self.parts, self.shape = parts, shape

    def copies(self, refs, dest, sems, first):
        out = []
        for i, (ref, (_, rows, r, c)) in enumerate(zip(refs, self.parts)):
            out.append(
                pltpu.make_async_copy(
                    ref.at[pl.ds(0, rows)],
                    dest.at[pl.ds(r, rows), pl.ds(c, ref.shape[1])],
                    sems.at[first + i],
                )
            )
        return out


def aligned(index, width):
    return pl.ds(pl.multiple_of(index, LANES), width)


def norm1(plan, meta, resid, gain):
    rows, width = resid.shape
    block = width // plan.fs

    def body(m, x_ref, g_ref, rel_ref, out_ref):
        data = x_ref[...].astype(F32)
        inv = lax.rsqrt(jnp.mean(data * data, axis=-1, keepdims=True) + 1e-06)
        for k in range(plan.fs):
            src = aligned(m[0, k] * block, block)
            x = x_ref[:, src]
            rel_ref[:, k * block : (k + 1) * block] = x
            out_ref[:, k * block : (k + 1) * block] = (x.astype(F32) * inv * g_ref[:, src]).astype(BF16)

    return call(body, meta, [(resid, False), (gain, False)], [(resid.shape, BF16)] * 2, [], resid.size * 8, "norm1")


def glu_kernel(plan, meta, pieces, value, gate, value_scale, gate_scale):
    tok, depth = pieces[0].shape
    width = value.shape[1]
    step = min(256, width)
    n = len(pieces)
    nv, ng = len(value.parts), len(gate.parts)

    def body(m, *refs):
        xs, refs = refs[:n], refs[n:]
        vs, gs, (vsc, gsc, out, xbuf, vbuf, gbuf, sems) = refs[:nv], refs[nv : nv + ng], refs[nv + ng :]
        weights = value.copies(vs, vbuf, sems, n) + gate.copies(gs, gbuf, sems, n + nv)
        loads = [pltpu.make_async_copy(xs[i], xbuf.at[i], sems.at[i]) for i in range(n)]
        for c in weights + loads:
            c.start()
        for c in weights:
            c.wait()
        first = m[0, plan.fs + plan.tp] * width
        for i in range(n):
            loads[i].wait()
            at = m[0, plan.fs + i] * tok

            def chunk(j, carry):
                cols = aligned(j * step, step)
                scols = aligned(first + j * step, step)
                x = xbuf[i]
                v = jnp.dot(x, vbuf[:, cols], preferred_element_type=F32) * vsc[:, scols]
                g = jnp.dot(x, gbuf[:, cols], preferred_element_type=F32) * gsc[:, scols]
                out[pl.ds(pl.multiple_of(at, 16), tok), cols] = (v * jax.nn.sigmoid(g)).astype(BF16)
                return carry

            lax.fori_loop(0, width // step, chunk, 0)

    ins = [(p, True) for p in pieces] + [(a, True) for a, *_ in value.parts + gate.parts]
    ins += [(value_scale, False), (gate_scale, False)]
    scratch = [
        pltpu.VMEM((n, tok, depth), BF16),
        pltpu.VMEM((depth, width), BF16),
        pltpu.VMEM((depth, width), BF16),
        pltpu.SemaphoreType.DMA((n + nv + ng,)),
    ]
    return call(body, meta, ins, [((n * tok, width), BF16)], scratch, 4 * n * tok * depth * width, "glu")[0]


def split3(x):
    hi = x.astype(BF16)
    rest = x - hi.astype(F32)
    mid = rest.astype(BF16)
    return hi, mid, (rest - mid.astype(F32)).astype(BF16)


def exact_dot(x, picks):
    return sum(jnp.dot(p, picks, preferred_element_type=F32) for p in split3(x))


def conv_kernel(plan, meta, glu, taps):
    length, width = glu.shape
    tok = length // plan.tp
    ntaps = taps.shape[0]
    reach = ntaps // 2
    front = -(-reach // 16) * 16
    lead = front - reach
    spans = (ntaps + lead - 1) // 8 + 1
    rows = 64
    padded = length + front + 8 * spans + 8

    def body(m, g_ref, t_ref, conv_ref, st_ref, pad, sums, squares):
        first = m[0, plan.fs + plan.tp] * width
        pad[0:front, :] = jnp.zeros((front, LANES), F32)
        pad[front + length :, :] = jnp.zeros((padded - front - length, LANES), F32)
        for b in range(width // LANES):
            cols = slice(b * LANES, (b + 1) * LANES)
            pad[front : front + length, :] = g_ref[:, cols].astype(F32)
            tcols = aligned(first + b * LANES, LANES)

            def chunk(i, carry):
                at = pl.multiple_of(i * rows, 8)
                total = None
                for r in range(8):
                    y = None
                    for q in range(spans):
                        j = 8 * q + r - lead
                        if not 0 <= j < ntaps:
                            continue
                        term = pad[pl.ds(at + 8 * q, rows + 8), :] * t_ref[j : j + 1, tcols]
                        y = term if y is None else y + term
                    if y is None:
                        continue
                    if r:
                        y = pltpu.roll(y, rows + 8 - r, 0)
                    total = y[:rows] if total is None else total + y[:rows]
                conv_ref[pl.ds(at, rows), cols] = total
                if b == 0:
                    sums[pl.ds(at, rows), :] = total
                    squares[pl.ds(at, rows), :] = total * total
                else:
                    sums[pl.ds(at, rows), :] += total
                    squares[pl.ds(at, rows), :] += total * total
                return carry

            lax.fori_loop(0, length // rows, chunk, 0)
        src = lax.broadcasted_iota(jnp.int32, (LANES, LANES), 0) % GROUPS
        dst = lax.broadcasted_iota(jnp.int32, (LANES, LANES), 1)
        pick_s = (src == dst).astype(BF16)
        pick_q = (src + GROUPS == dst).astype(BF16)
        for t in range(plan.tp):
            sl = slice(t * tok, (t + 1) * tok)
            both = exact_dot(sums[sl, :], pick_s) + exact_dot(squares[sl, :], pick_q)
            st_ref[t] = both.T[: 2 * GROUPS]

    scratch = [pltpu.VMEM((padded, LANES), F32), pltpu.VMEM((length, LANES), F32), pltpu.VMEM((length, LANES), F32)]
    outs = [((length, width), F32), ((plan.tp, 2 * GROUPS, tok), F32)]
    flops = 80 * length * width * 60
    return call(body, meta, [(glu, False), (taps, False)], outs, scratch, flops, "conv")


def point_kernel(plan, meta, which, conv, stats, gain, point, channels, name):
    length, width = conv.shape
    tok = length // plan.tp
    depth = point.shape[1]
    step = min(512, depth)
    ns, np_ = len(stats), len(point.parts)

    def body(m, conv_ref, *refs):
        sts, refs = refs[:ns], refs[ns:]
        ps, (g_ref, out, cbuf, abuf, wbuf, sems) = refs[:np_], refs[np_:]
        idx = m[0, plan.fs + which]
        load = pltpu.make_async_copy(conv_ref.at[pl.ds(pl.multiple_of(idx * tok, 16), tok)], cbuf, sems.at[0])
        load.start()
        weights = point.copies(ps, wbuf, sems, 1)
        for c in weights:
            c.start()
        tot = sts[0][idx]
        for s in sts[1:]:
            tot = tot + s[idx]
        tot = tot * (1.0 / (channels // GROUPS))
        gm, gs = tot[:GROUPS], tot[GROUPS:]
        inv = lax.rsqrt(gs - gm * gm + 1e-05)
        packed = jnp.concatenate([gm, inv, jnp.zeros((LANES - 2 * GROUPS, tok), F32)], axis=0).T
        src = lax.broadcasted_iota(jnp.int32, (LANES, LANES), 0)
        dst = lax.broadcasted_iota(jnp.int32, (LANES, LANES), 1) % GROUPS
        gm_all = exact_dot(packed, (src == dst).astype(BF16))
        inv_all = exact_dot(packed, (src == dst + GROUPS).astype(BF16))
        first = m[0, plan.fs + plan.tp] * width
        load.wait()
        for b in range(width // LANES):
            cols = slice(b * LANES, (b + 1) * LANES)
            v = (cbuf[:, cols] - gm_all) * inv_all * g_ref[:, aligned(first + b * LANES, LANES)]
            abuf[:, cols] = (v / (1.0 + jnp.exp(-v))).astype(BF16)
        for c in weights:
            c.wait()

        def chunk(j, carry):
            cols = aligned(j * step, step)
            out[:, cols] = jnp.dot(abuf[...], wbuf[:, cols], preferred_element_type=F32).astype(BF16)
            return carry

        lax.fori_loop(0, depth // step, chunk, 0)

    ins = [(conv, True)] + [(s, False) for s in stats] + [(a, True) for a, *_ in point.parts] + [(gain, False)]
    scratch = [
        pltpu.VMEM((tok, width), F32),
        pltpu.VMEM((tok, width), BF16),
        pltpu.VMEM((width, depth), BF16),
        pltpu.SemaphoreType.DMA((1 + np_,)),
    ]
    return call(body, meta, ins, [((tok, depth), BF16)], scratch, 2 * tok * depth * width, name)[0]


def middle_kernel(plan, meta, resid_rel, terms, scales, gain):
    rows, width = resid_rel.shape
    block = width // plan.fs
    n = len(terms)

    def body(m, x_ref, *refs):
        ts, (s_ref, g_ref, mid_ref, out_ref) = refs[:n], refs[n:]
        total = ts[0][...].astype(F32)
        for t in ts[1:]:
            total = total + t[...].astype(F32)
        mid = (x_ref[...].astype(F32) + total * s_ref[0:1, :]).astype(BF16)
        mid_ref[...] = mid
        data = mid.astype(F32)
        inv = lax.rsqrt(jnp.mean(data * data, axis=-1, keepdims=True) + 1e-06)
        for k in range(plan.fs):
            own = slice(k * block, (k + 1) * block)
            out_ref[:, own] = (mid_ref[:, own].astype(F32) * inv * g_ref[:, aligned(m[0, k] * block, block)]).astype(BF16)

    ins = [(resid_rel, False)] + [(t, False) for t in terms] + [(scales, False), (gain, False)]
    return call(body, meta, ins, [(resid_rel.shape, BF16)] * 2, [], resid_rel.size * 8, "middle")


def up_kernel(plan, meta, pieces, up, up_scale, name):
    tok, depth = pieces[0].shape
    width = up.shape[1]
    step = min(512, width)
    n, nu = len(pieces), len(up.parts)

    def body(m, *refs):
        xs, us, (s_ref, *rest) = refs[:n], refs[n : n + nu], refs[n + nu :]
        outs, (xbuf, ubuf, sems) = rest[:n], rest[n:]
        weights = up.copies(us, ubuf, sems, n)
        loads = [pltpu.make_async_copy(xs[i], xbuf.at[i], sems.at[i]) for i in range(n)]
        for c in loads + weights:
            c.start()
        for c in weights:
            c.wait()
        for i in range(n):
            loads[i].wait()

            def chunk(j, carry):
                cols = aligned(j * step, step)
                h = jnp.dot(xbuf[i], ubuf[:, cols], preferred_element_type=F32) * s_ref[:, cols]
                h = jnp.maximum(h, 0.0)
                outs[i][:, cols] = (h * h).astype(BF16)
                return carry

            lax.fori_loop(0, width // step, chunk, 0)

    ins = [(p, True) for p in pieces] + [(a, True) for a, *_ in up.parts] + [(up_scale, False)]
    scratch = [
        pltpu.VMEM((n, tok, depth), BF16),
        pltpu.VMEM((depth, width), BF16),
        pltpu.SemaphoreType.DMA((n + nu,)),
    ]
    return call(body, meta, ins, [((tok, width), BF16)] * n, scratch, 2 * n * tok * depth * width, name)


def down_kernel(plan, meta, hidden, down, name):
    tok, depth = hidden[0].shape
    width = down.shape[1]
    n, nd = len(hidden), len(down.parts)

    def body(m, *refs):
        xs, ds, (keep, give, xbuf, dbuf, sems) = refs[:n], refs[n : n + nd], refs[n + nd :]
        weights = down.copies(ds, dbuf, sems, n)
        loads = [pltpu.make_async_copy(xs[i], xbuf.at[i], sems.at[i]) for i in range(n)]
        for c in weights + loads:
            c.start()
        for c in weights:
            c.wait()
        for i in range(n):
            loads[i].wait()
            out = give if i % 2 else keep
            for j in range(0, width, 256):
                cols = slice(j, min(j + 256, width))
                out[i // 2, :, cols] = jnp.dot(xbuf[i], dbuf[:, cols], preferred_element_type=F32).astype(BF16)

    ins = [(h, True) for h in hidden] + [(a, True) for a, *_ in down.parts]
    scratch = [
        pltpu.VMEM((n, tok, depth), BF16),
        pltpu.VMEM((depth, width), BF16),
        pltpu.SemaphoreType.DMA((n + nd,)),
    ]
    outs = [((n // 2, tok, width), BF16)] * 2
    return call(body, meta, ins, outs, scratch, 2 * n * tok * depth * width, name)


def final_kernel(plan, meta, middle, chunks, scales):
    rows, width = middle.shape
    block = width // plan.fs
    flat = [t for _, terms in chunks for t in terms]
    n = len(flat)

    def body(m, mid_ref, *refs):
        ts, (s_ref, out) = refs[:n], refs[n:]
        at = 0
        for first, terms in chunks:
            for j in range(0, terms[0].shape[-1], block):
                total = None
                for i in range(len(terms)):
                    t = ts[at + i][0, :, j : j + block].astype(F32)
                    total = t if total is None else total + t
                own = slice(first + j, first + j + block)
                value = mid_ref[:, own].astype(F32) + total * s_ref[1:2, own]
                out[:, aligned(m[0, (first + j) // block] * block, block)] = value.astype(BF16)
            at += len(terms)

    ins = [(middle, False)] + [(t, False) for t in flat] + [(scales, False)]
    return call(body, meta, ins, [(middle.shape, BF16)], [], middle.size * 8, "final")[0]


def after(x, gate):
    return lax.optimization_barrier((x, *gate))[0] if gate else x


class Ring:
    def __init__(self, plan, shard, cut, gate, name):
        with jax.named_scope(name):
            shard = after(shard, gate)
            self.whole = [shard]
            fwd = bwd = shard
            for _ in range(1, plan.hops):
                fwd = lax.ppermute(fwd, "fs", plan.fwd)
                bwd = lax.ppermute(bwd, "fs", plan.bwd)
                self.whole += [fwd, bwd]
            self.gate = (fwd, bwd)
            self.halves = (lax.ppermute(fwd[:cut], "fs", plan.fwd), lax.ppermute(bwd[cut:], "fs", plan.bwd))
            self.cut = cut

    def parts(self, slot, rows, r, c):
        if slot < len(self.whole):
            return [(self.whole[slot], rows, r, c)]
        return [(self.halves[0], self.cut, r, c), (self.halves[1], rows - self.cut, r + self.cut, c)]


def shards(
    plan,
    resid,
    norm1_gain,
    w_value,
    w_gate,
    value_scale,
    gate_scale,
    conv_taps,
    conv_gain,
    w_point,
    point_scale,
    norm2_gain,
    w_up,
    up_scale,
    w_down,
    down_scale,
):
    tok, width = resid.shape
    channels = value_scale.shape[0]
    fs, chips = plan.fs, plan.chips
    row = lax.axis_index("fs") * plan.tp + lax.axis_index("tp")
    meta = lax.dynamic_slice_in_dim(jnp.asarray(plan.table()), row, 1, 0)
    swap = functools.partial(lax.ppermute, axis_name="tp", perm=plan.core_swap)

    def flat(v):
        return v.reshape(1, -1)

    vrows, own_width = w_value.shape
    shard = point_scale.shape[0]
    pair = jnp.concatenate([point_scale, down_scale])
    hi = lax.reduce_precision(pair, 8, 7)
    mid = lax.reduce_precision(pair - hi, 8, 7)
    extra = 16 * -(-(6 * shard) // (16 * own_width))
    tail = jnp.pad(jnp.concatenate([hi, mid, pair - hi - mid]), (0, extra * own_width - 6 * shard))
    carried = jnp.concatenate([w_value.astype(BF16), tail.reshape(extra, own_width).astype(BF16)], axis=0)
    ucut = 3 * w_up.shape[1] // 8
    dcut = w_down.shape[0] // 2
    ring_v = Ring(plan, carried, vrows // 2, (), "ring_v")
    ring_g = Ring(plan, w_gate.astype(BF16), vrows // 2, (), "ring_g")
    ring_p = Ring(plan, w_point.astype(BF16), w_point.shape[0] // 2, ring_v.gate, "ring_p")
    up_bf = w_up.astype(BF16)
    ring_u1 = Ring(plan, up_bf[:, ucut:], vrows // 2, ring_g.gate, "ring_u1")
    ring_u0 = Ring(plan, up_bf[:, :ucut], vrows // 2, ring_p.gate, "ring_u0")
    down_bf = w_down.astype(BF16)
    ring_d0 = Ring(plan, down_bf[:dcut], dcut // 2, ring_u0.gate, "ring_d0")
    ring_d1 = Ring(plan, down_bf[dcut:], dcut // 2, ring_u1.gate, "ring_d1")

    def rows_of(ring, w, c=0):
        return [p for k in range(fs) for p in ring.parts(k, vrows, k * vrows, c)]

    value = Parts(rows_of(ring_v, own_width), (width, own_width))
    gate = Parts(rows_of(ring_g, own_width), (width, own_width))
    point = Parts(
        [p for k in range(fs) for p in ring_p.parts(k, w_point.shape[0], 0, k * shard)], (w_point.shape[0], width)
    )
    up = Parts(rows_of(ring_u0, ucut) + rows_of(ring_u1, ucut, ucut), (width, w_up.shape[1]))
    tails = [b[vrows:] for b in ring_v.whole] + [ring_v.halves[1][vrows - vrows // 2 :]]
    pieces = jnp.stack(tails).astype(F32).reshape(fs, -1)[:, : 6 * shard].reshape(fs, 3, 2, shard)
    scales = jnp.transpose(jnp.sum(pieces, axis=1), (1, 0, 2)).reshape(2, width)

    def gather(x, name):
        with jax.named_scope(name):
            same, other = [x], [swap(x)]
            away = {}
            for d in range(1, chips):
                away[(chips - d) % chips] = lax.ppermute(x, "tp", plan.shift(d))
            for s in range(1, chips):
                same.append(away[s])
                other.append(swap(away[s]))
        return [p for pair in zip(same, other) for p in pair]

    resid_rel, normed = norm1(plan, meta, resid, flat(norm1_gain))
    tokens = gather(normed, "gather1")
    glu = glu_kernel(plan, meta, tokens, value, gate, flat(value_scale), flat(gate_scale))
    conv, own_stats = conv_kernel(plan, meta, glu, conv_taps)
    with jax.named_scope("stats"):
        chip_stats = own_stats + swap(own_stats)
        stats = [chip_stats] + [lax.ppermute(chip_stats, "tp", plan.shift(d)) for d in range(1, chips)]

    def piece(which, name):
        return point_kernel(plan, meta, which, conv, stats, flat(conv_gain), point, channels, name)

    terms = []
    for s in list(range(1, chips)) + [0]:
        give = piece(2 * s + 1, "point_give%d" % s)
        keep = piece(2 * s, "point_keep%d" % s)
        with jax.named_scope("scatter1_%d" % s):
            got = swap(give)
            if s:
                both = (keep.astype(F32) + got.astype(F32)).astype(BF16)
                terms.append(lax.ppermute(both, "tp", plan.shift(s)))
            else:
                terms += [keep, got]
    middle, normed2 = middle_kernel(plan, meta, resid_rel, terms, scales, flat(norm2_gain))
    tokens2 = gather(normed2, "gather2")
    hidden = []
    for s in range(chips):
        hidden += up_kernel(plan, meta, tokens2[2 * s : 2 * s + 2], up, flat(up_scale), "up%d" % s)

    groups = [list(range(min(3, fs - 1)))]
    groups += [[k, k + 1] for k in range(3, fs - 1, 2)] + [[fs - 1]]
    chunks = []
    for i, slots in enumerate(groups):
        blocks = []
        for j, k in enumerate(slots):
            blocks += ring_d0.parts(k, dcut, 0, j * shard) + ring_d1.parts(k, w_down.shape[0] - dcut, dcut, j * shard)
        down = Parts(blocks, (w_down.shape[0], len(slots) * shard))
        keep, give = down_kernel(plan, meta, hidden, down, "down%d" % i)
        with jax.named_scope("scatter2_%d" % i):
            got = swap(give)
            here = [keep, got]
            if chips > 1:
                both = (keep[1:].astype(F32) + got[1:].astype(F32)).astype(BF16)
                here += [lax.ppermute(both[s - 1 : s], "tp", plan.shift(s)) for s in range(1, chips)]
        chunks.append((slots[0] * shard, here))
    return final_kernel(plan, meta, middle, chunks, scales)


def solution(mesh):
    plan = Plan(mesh.shape["fs"], mesh.shape["tp"])
    in_specs = (
        P(("fs", "tp"), None),
        P(),
        P("fs", "tp"),
        P("fs", "tp"),
        P(),
        P(),
        P(),
        P(),
        P("tp", "fs"),
        P("fs"),
        P(),
        P("fs", "tp"),
        P("tp"),
        P("tp", "fs"),
        P("fs"),
    )
    out_specs = P(("fs", "tp"), None)
    return jax.shard_map(
        functools.partial(shards, plan), mesh=mesh, in_specs=in_specs, out_specs=out_specs, check_vma=False
    )
```
